512 devices in a mesh: sp: 128 (over z, x, core), tp: 4 (over y).
Axes of the slice: x: 4, y: 4, z: 16, core: 2. Of those that a mesh axis runs over, the one named last changes fastest.
Arguments:
- inputs: bfloat16 [4, 16384, 1024], P(None, 'sp'), may hold values from -6 to 6
- norm_gain: float32 [1024], replicated, may hold values from 0.1 to 1.9
- query_weight: bfloat16 [1024, 3, 8, 64], P('sp', None, 'tp'), may hold values from -0.1875 to 0.1875
- key_weight: bfloat16 [1024, 3, 8, 64], P('sp', None, 'tp'), may hold values from -0.1875 to 0.1875
- value_weight: bfloat16 [1024, 3, 8, 64], P('sp', None, 'tp'), may hold values from -0.1875 to 0.1875
- query_gain: float32 [3, 64], replicated, may hold values from 0.1 to 1.9
- key_gain: float32 [3, 64], replicated, may hold values from 0.1 to 1.9
- out_weight: bfloat16 [8, 64, 1024], P('tp', None, 'sp'), may hold values from -0.75 to 0.75
Outputs:
- mixed: bfloat16 [4, 16384, 1024], P(None, 'sp', 'tp')
The draws below stay inside these ranges and needn't reach their ends.
All inputs are finite; a program needn't handle non-finite values.
Results may differ from the reference program's by a relative error of at most 0.02.
Values may be sent and summed in bfloat16 or wider, within the bound.
A program may use at most 64 MiB of HBM per device.

```python
import math
import jax
import jax.numpy as jnp
from jax import lax

D = 1024
GROUPS = 3
HPG = 8
DH = 64
BATCH = 4
SPAN_CLOSE = 32
SPREAD_CENTRAL = 4
SPAN_CENTRAL = 32
SPREAD_DISTANT = 16
SPAN_DISTANT = 16
TOKENS = 16384


def level_of(key, dims, split, least, largest):
    def one(position, shards_of):
        heights = jax.random.uniform(jax.random.fold_in(jax.random.fold_in(key, 6), position), (shards_of,), jnp.float32, least / len(split), largest / len(split))
        return jnp.repeat(jnp.exp(heights), dims[position] // shards_of).reshape((-1,) + (1,) * (len(dims) - position - 1))

    factor_of = one(*split[0])
    for cut in split[1:]:
        factor_of = factor_of * one(*cut)
    return factor_of


def centred(key, extent, deviation, bound, cuts=(), kind=jnp.bfloat16):
    drawn = deviation * jax.random.normal(key, extent, jnp.float32)
    if cuts:
        drawn = drawn * level_of(key, extent, cuts, -0.22, 0.18)
    return jnp.clip(drawn, -bound, bound).astype(kind)


def setup_inputs(seed: int = 0) -> dict:
    key_of = jax.random.split(jax.random.key(seed), 9)
    inputs = centred(key_of[0], (BATCH, TOKENS, D), 1.0, 6.0, ((1, 128),))
    norm_gain = jnp.clip(1.0 + 0.18 * jax.random.normal(key_of[1], (D,), jnp.float32), 0.1, 1.9)
    query_weight = centred(key_of[2], (D, GROUPS, HPG, DH), D ** -0.5, 0.1875, ((0, 128), (2, 4)))
    key_weight = centred(key_of[3], (D, GROUPS, HPG, DH), D ** -0.5, 0.1875, ((0, 128), (2, 4)))
    value_weight = centred(key_of[4], (D, GROUPS, HPG, DH), D ** -0.5, 0.1875, ((0, 128), (2, 4)))
    query_gain = jnp.clip(1.0 + 0.18 * jax.random.normal(key_of[5], (GROUPS, DH), jnp.float32), 0.1, 1.9)
    key_gain = jnp.clip(1.0 + 0.18 * jax.random.normal(key_of[6], (GROUPS, DH), jnp.float32), 0.1, 1.9)
    out_weight = centred(key_of[7], (HPG, DH, D), DH ** -0.5, 0.75, ((0, 4), (2, 128)))
    return dict(inputs=inputs, norm_gain=norm_gain, query_weight=query_weight, key_weight=key_weight, value_weight=value_weight, query_gain=query_gain, key_gain=key_gain, out_weight=out_weight)


eps = 1e-06
neg_fill = -1e+30
block_rows = 128

def row_norm(values, gain):
    scaled = values * lax.rsqrt(lax.optimization_barrier(jnp.mean(values * values, axis=-1, keepdims=True)) + eps)
    return scaled * gain

def band_attend(queries, keys, values, dilation, half, slopes):
    seq_len, heads, width = queries.shape
    sub_len = seq_len // dilation

    def to_sub(tensor):
        return tensor.reshape(sub_len, dilation, heads, width).transpose(1, 0, 2, 3)
    query_sub = to_sub(queries)
    key_sub = to_sub(keys)
    value_sub = to_sub(values)
    blocks = -(-sub_len // block_rows)
    padded_len = blocks * block_rows
    key_rows = block_rows + 2 * half
    query_sub = jnp.pad(query_sub, ((0, 0), (0, padded_len - sub_len), (0, 0), (0, 0)))
    key_pad = ((0, 0), (half, padded_len - sub_len + half), (0, 0), (0, 0))
    key_sub = jnp.pad(key_sub, key_pad)
    value_sub = jnp.pad(value_sub, key_pad)
    key_index = jnp.arange(blocks)[:, None] * block_rows + jnp.arange(key_rows)[None, :]
    key_blocks = key_sub[:, key_index]
    value_blocks = value_sub[:, key_index]
    query_blocks = query_sub.reshape(dilation, blocks, block_rows, heads, width)
    scores = jnp.einsum('nbqhe,nbkhe->nbhqk', query_blocks, key_blocks, precision=lax.Precision.HIGHEST) / math.sqrt(width)
    offset = jnp.arange(key_rows)[None, :] - half - jnp.arange(block_rows)[:, None]
    key_place = key_index - half
    allowed = (jnp.abs(offset)[None] <= half) & ((key_place >= 0) & (key_place < sub_len))[:, None, :]
    slant = -slopes[:, None, None] * (jnp.abs(offset).astype(jnp.float32) / float(half))[None]
    scores = jnp.where(allowed[None, :, None], scores + slant[None, None], neg_fill)
    log_total = jax.nn.logsumexp(scores, axis=-1)
    weights = jnp.exp(scores - log_total[..., None])
    result = jnp.einsum('nbhqk,nbkhe->nbqhe', weights, value_blocks, precision=lax.Precision.HIGHEST).reshape(dilation, padded_len, heads, width)[:, :sub_len]
    log_total = log_total.transpose(0, 1, 3, 2).reshape(dilation, padded_len, heads)[:, :sub_len]
    result = result.transpose(1, 0, 2, 3).reshape(seq_len, heads, width)
    log_total = log_total.transpose(1, 0, 2).reshape(seq_len, heads)
    return (result, log_total)

def reference(inputs, norm_gain, query_weight, key_weight, value_weight, query_gain, key_gain, out_weight):
    batch, seq_len, model_width = inputs.shape
    groups = query_weight.shape[1]
    heads = query_weight.shape[2]
    head_width = query_weight.shape[3]
    normed = row_norm(inputs.astype(jnp.float32), norm_gain).astype(jnp.bfloat16)
    normed = normed.reshape(batch * seq_len, model_width)

    def project(weight):
        product = jnp.dot(normed, weight.reshape(model_width, -1), preferred_element_type=jnp.float32)
        return product.astype(jnp.bfloat16).reshape(batch, seq_len, groups, heads, head_width)
    queries = project(query_weight)
    keys = project(key_weight)
    values = project(value_weight)
    slopes = jnp.exp2(-8.0 * jnp.arange(1, heads + 1).astype(jnp.float32) / heads)
    gap_layouts = ((1, SPAN_CLOSE), (SPREAD_CENTRAL, SPAN_CENTRAL), (SPREAD_DISTANT, SPAN_DISTANT))
    results = []
    totals = []
    for group in range(3):
        dilation, half = gap_layouts[group]
        query_group = row_norm(queries[:, :, group].astype(jnp.float32), query_gain[group])
        key_group = row_norm(keys[:, :, group].astype(jnp.float32), key_gain[group])
        value_group = values[:, :, group].astype(jnp.float32)

        def attend_one(trio, dilation=dilation, half=half):
            return band_attend(trio[0], trio[1], trio[2], dilation, half, slopes)
        result, log_total = lax.map(attend_one, (query_group, key_group, value_group))
        results.append(result)
        totals.append(log_total)
    weights = jax.nn.softmax(jnp.stack(totals, 0), axis=0)
    combined = lax.optimization_barrier(jnp.sum(weights[..., None] * jnp.stack(results, 0), axis=0))
    merged = combined.astype(jnp.bfloat16).reshape(batch * seq_len, heads * head_width)
    output = jnp.dot(merged, out_weight.reshape(heads * head_width, model_width), preferred_element_type=jnp.float32)
    return output.astype(jnp.bfloat16).reshape(batch, seq_len, model_width)
```

```python
import functools
import math

import jax
import jax.numpy as jnp
from jax import lax
from jax.experimental import pallas as pl
from jax.experimental.pallas import tpu as pltpu
from jax.sharding import Mesh
from jax.sharding import PartitionSpec as P

REACH = (32, 128, 256)
SPREAD = (1, 4, 16)
eps = 1e-06
SP = ("z", "x", "c")
bf16 = jnp.bfloat16
f32 = jnp.float32


def kernel(
    Z, X, Y, L, inputs, weights, norm_gain, gains, out,
    xbuf, wbuf, wfull, xn, qbuf, kv0, kv1, kv2, valid, m0, m1, m2, mout, mbuf, wo,
    x_send, x_recv, in_send, in_recv, in_local,
    r_send, r_recv, l_send, l_recv, dr_send, dr_recv, dl_send, dl_recv,
    h_send, h_recv, o_send, o_recv, y_send, y_recv,
):
    kv = (kv0, kv1, kv2)
    mask = (m0, m1, m2)
    z, x, c, y = (lax.axis_index(a) for a in ("z", "x", "c", "y"))
    half_x = X // 2
    H = Z // 2
    D = Z * X * 16
    rows = X * L
    cols = D // Y
    wide = 1152

    def at(dz=0, dx=0, dc=0, dy=0):
        return {
            "z": lax.rem(z + dz + Z, Z),
            "x": lax.rem(x + dx + X, X),
            "c": lax.rem(c + dc, 2),
            "y": lax.rem(y + dy + Y, Y),
        }

    def remote(src, dst, send, recv, target):
        return pltpu.make_async_remote_copy(
            src_ref=src, dst_ref=dst, send_sem=send, recv_sem=recv,
            device_id=target, device_id_type=pl.DeviceIdType.MESH,
        )

    barrier = pltpu.get_barrier_semaphore()
    count = 0
    for dx in range(X):
        for dc in range(2):
            for dy in range(Y):
                if dx or dc or dy:
                    pl.semaphore_signal(
                        barrier, inc=1, device_id=at(0, dx, dc, dy),
                        device_id_type=pl.DeviceIdType.MESH,
                    )
                    count += 1
    cross = 2 * c - 1
    for target in (at(1), at(-1), at(cross, 0, 1)):
        pl.semaphore_signal(barrier, inc=1, device_id=target, device_id_type=pl.DeviceIdType.MESH)
        count += 1
    pl.semaphore_wait(barrier, count)

    def x_copy(j):
        return remote(weights, wbuf.at[c, z, x], x_send.at[j], x_recv.at[j], at(0, j))

    def slot(zz, j):
        return wbuf.at[c, lax.rem(zz + 2 * Z, Z), lax.rem(x + j, X)]

    def r_copy(k, j, first=False):
        s = slot(z - k, j)
        return remote(weights if first else s, s, r_send.at[k, j], r_recv.at[k, j], at(1))

    def l_copy(k, j, first=False):
        s = slot(z + k, j)
        return remote(weights if first else s, s, l_send.at[k, j], l_recv.at[k, j], at(-1))

    def dr_copy(k):
        s = wbuf.at[c, lax.rem(z - k + Z, Z)]
        return remote(s, s, dr_send.at[k], dr_recv.at[k], at(0, 0, 1))

    def dl_copy(k):
        s = wbuf.at[c, lax.rem(z + k, Z)]
        return remote(s, s, dl_send.at[k], dl_recv.at[k], at(0, 0, 1))

    r_copy(0, 0, True).start()
    l_copy(0, 0, True).start()
    for j in range(1, X):
        x_copy(j).start()

    mine = x // half_x
    place = lax.rem(x, half_x) * 2 + c

    def in_copy(j):
        b = lax.rem(x + j, X)
        target = {"z": z, "x": b, "c": mine, "y": y}
        return remote(inputs.at[b], xbuf.at[place], in_send.at[j], in_recv.at[place], target)

    own_copy = pltpu.make_async_copy(inputs.at[x], xbuf.at[place], in_local)

    @pl.when(mine == c)
    def _():
        own_copy.start()

    @pl.when(mine != c)
    def _():
        in_copy(0).start()

    for j in range(1, X):
        in_copy(j).start()

    wbuf[c, z, x] = weights[...]

    lane = lax.broadcasted_iota(jnp.int32, (1, 128), 1)
    low = lane < 64

    def masks(step):
        size = L // H
        start = pl.multiple_of(step * size, size)
        for g in range(3):
            reach, spread = REACH[g], SPREAD[g]
            shape = (size, L + 2 * reach)
            gap = (
                lax.broadcasted_iota(jnp.int32, shape, 1)
                - lax.broadcasted_iota(jnp.int32, shape, 0)
                - reach
                - start
            )
            far = jnp.abs(gap)
            ok = (far <= reach) & ((gap & (spread - 1)) == 0)
            far = far.astype(f32) * (1.0 / reach)
            for h in range(2):
                order = jnp.full((size, 128), 2 * y + h + 1, jnp.int32).astype(f32)
                slope = jnp.exp2(order * (-8.0 / (2 * Y)))[:, :1]
                mask[g][h, pl.ds(start, size), :] = jnp.where(ok, jnp.exp(-slope * far), 0.0)

    def combine(zz):
        zz = lax.rem(zz + 2 * Z, Z)
        for j in range(X):
            both = jnp.concatenate(
                [wbuf[0, zz, j].astype(f32), wbuf[1, zz, j].astype(f32)], axis=0
            )
            spot = pl.multiple_of((zz * X + j) * 16, 16)
            wfull[pl.ds(spot, 16), :] = both.astype(bf16)

    for j in range(1, X):
        x_copy(X - j).wait_recv()
        r_copy(0, j).start()
        l_copy(0, j).start()
    dr_copy(0).start()
    masks(0)
    place_key = (2 * z + c) * rows - REACH[2] + lax.broadcasted_iota(
        jnp.int32, (rows + 2 * REACH[2], 128), 0
    )
    inside = (place_key >= 0) & (place_key < 2 * Z * rows)
    valid[...] = jnp.where(inside, 1.0, 0.0).astype(bf16)

    def ring(k, carry):
        for j in range(X):
            r_copy(k - 1, j).wait_recv()
            r_copy(k, j).start()
            l_copy(k - 1, j).wait_recv()

            @pl.when(k < H - 1)
            def _():
                l_copy(k, j).start()

        dr_copy(k).start()
        dl_copy(k).start()
        masks(k)
        dr_copy(k - 1).wait_recv()
        combine(z - k + 1)

        @pl.when(k > 1)
        def _():
            dl_copy(k - 1).wait_recv()
            combine(z + k - 1)

        return carry

    lax.fori_loop(1, H, ring, 0)
    for j in range(X):
        r_copy(H - 1, j).wait_recv()
    dr_copy(H).start()
    dr_copy(H - 1).wait_recv()
    combine(z - H + 1)
    dl_copy(H - 1).wait_recv()
    combine(z + H - 1)

    for k in range(X):
        @pl.when((mine == c) & (place == k))
        def _():
            own_copy.wait()

        @pl.when((mine != c) | (place != k))
        def _():
            remote(inputs.at[0], xbuf.at[k], in_send.at[0], in_recv.at[k], at(0, 1)).wait_recv()

        value = xbuf[k].astype(f32)
        mean = jnp.mean(value * value, axis=-1, keepdims=True)
        xn[pl.ds(k * L, L), :] = (value * lax.rsqrt(mean + eps) * norm_gain[...]).astype(bf16)

    dr_copy(H).wait_recv()
    combine(z - H)

    def y_copy(j):
        t = lax.rem(y + j, Y)
        spot = pl.multiple_of(t * cols, cols)
        return remote(
            wfull.at[pl.ds(spot, cols), pl.ds(wide, 128)], wo.at[y],
            y_send.at[j], y_recv.at[j], at(0, 0, 0, j),
        )

    for j in range(1, Y):
        y_copy(j).start()
    wo[y] = wfull[pl.ds(pl.multiple_of(y * cols, cols), cols), wide:]

    chain = 2 * z + c
    has_left = chain > 0
    has_right = chain < 2 * Z - 1
    left = {"z": lax.rem(z + c - 1 + Z, Z), "x": x, "c": 1 - c, "y": y}
    right = {"z": lax.rem(z + c, Z), "x": x, "c": 1 - c, "y": y}
    same = (
        (lax.broadcasted_iota(jnp.int32, (128, 128), 0) < 64)
        == (lax.broadcasted_iota(jnp.int32, (128, 128), 1) < 64)
    )
    pick = jnp.where(same, 1.0, 0.0).astype(bf16)

    def to_right(g):
        reach = REACH[g]
        return remote(
            kv[g].at[:, pl.ds(rows, reach), :], kv[g].at[:, pl.ds(0, reach), :],
            h_send.at[g, 0], h_recv.at[g, 0], right,
        )

    def to_left(g):
        reach = REACH[g]
        return remote(
            kv[g].at[:, pl.ds(reach, reach), :], kv[g].at[:, pl.ds(reach + rows, reach), :],
            h_send.at[g, 1], h_recv.at[g, 1], left,
        )

    for g in (2, 1, 0):
        reach = REACH[g]

        def project(i, carry, g=g, reach=reach):
            start = pl.multiple_of(i * 256, 256)
            block = jnp.dot(
                xn[pl.ds(start, 256), :], wfull[:, g * 384 : (g + 1) * 384],
                preferred_element_type=f32,
            ).astype(bf16).astype(f32)
            for t in range(3):
                part = block[:, t * 128 : (t + 1) * 128]
                square = part * part
                high = square.astype(bf16)
                rest = (square - high.astype(f32)).astype(bf16)
                total = jnp.dot(high, pick, preferred_element_type=f32) + jnp.dot(
                    rest, pick, preferred_element_type=f32
                )
                scaled = part * (
                    lax.rsqrt(total * (1.0 / 64) + eps) * gains[pl.ds(g * 3 + t, 1), :]
                )
                if t == 0:
                    qbuf[g, pl.ds(start, 256), :] = scaled.astype(bf16)
                else:
                    chosen = jnp.where(low if t == 2 else ~low, scaled, part)
                    kv[g][t - 1, pl.ds(start + reach, 256), :] = chosen.astype(bf16)
            return carry

        lax.fori_loop(0, rows // 256, project, 0)

        @pl.when(has_right)
        def _():
            to_right(g).start()

        @pl.when(has_left)
        def _():
            to_left(g).start()

        @pl.when(jnp.logical_not(has_left))
        def _():
            kv[g][:, pl.ds(0, reach), :] = jnp.zeros((2, reach, 128), bf16)

        @pl.when(jnp.logical_not(has_right))
        def _():
            kv[g][:, pl.ds(reach + rows, reach), :] = jnp.zeros((2, reach, 128), bf16)

    for g in (2, 1, 0):
        @pl.when(has_left)
        def _():
            to_right(g).wait_recv()

        @pl.when(has_right)
        def _():
            to_left(g).wait_recv()

    def o_copy(k, j):
        target = {
            "z": z, "x": c * half_x + k // 2, "c": lax.rem(k, 2), "y": lax.rem(y + j, Y)
        }
        return remote(
            mout.at[k], mbuf.at[y, x], o_send.at[k, j], o_recv.at[y, x], target
        )

    def is_own(k):
        return (c * half_x + k // 2 == x) & (lax.rem(k, 2) == c)

    def attend(k, carry):
        base = pl.multiple_of(k * L, L)
        sums = []
        for h in range(2):
            total = jnp.zeros((L, 256), f32)
            for g in range(3):
                reach = REACH[g]
                span = L + 2 * reach
                query = qbuf[g, pl.ds(base, L), :]
                query = jnp.where(low if h == 1 else ~low, query, jnp.zeros_like(query))
                pair = kv[g][h, pl.ds(base, span), :]
                score = lax.dot_general(
                    query, pair, (((1,), (1,)), ((), ())), preferred_element_type=f32
                )
                weight = (jnp.exp2(score) * mask[g][h]).astype(bf16)
                ones = valid[pl.ds(base + REACH[2] - reach, span), :]
                total += jnp.dot(
                    weight, jnp.concatenate([pair, ones], axis=1), preferred_element_type=f32
                )
            sums.append(total[:, :128] / total[:, 128:])
        merged = jnp.where(low, sums[0], sums[1]).astype(bf16)
        mout[k] = merged

        @pl.when(is_own(k))
        def _():
            mbuf[y, x] = merged

        @pl.when(jnp.logical_not(is_own(k)))
        def _():
            o_copy(k, 0).start()

        for j in range(1, Y):
            o_copy(k, j).start()
        return carry

    lax.fori_loop(0, X, attend, 0)

    for j in range(1, Y):
        y_copy(Y - j).wait_recv()

    total = None
    for j in range(Y):
        t = lax.rem(y + j, Y)
        for b in range(X):
            def arrive():
                remote(mout.at[0], mbuf.at[t, b], o_send.at[0, 0], o_recv.at[t, b], at(0, 1)).wait_recv()

            if j == 0:
                pl.when((b != x) | (mine != c))(arrive)
            else:
                arrive()
        part = lax.dot_general(
            mbuf[t].reshape(X * L, 128), wo[t], (((1,), (1,)), ((), ())),
            preferred_element_type=f32,
        )
        total = part if total is None else total + part
    out[...] = total.reshape(X, L, cols).astype(bf16)

    for j in range(1, X):
        x_copy(j).wait_send()
        in_copy(j).wait_send()

    @pl.when(mine != c)
    def _():
        in_copy(0).wait_send()

    def sent(k, carry):
        for j in range(X):
            r_copy(k, j).wait_send()

            @pl.when(k < H - 1)
            def _():
                l_copy(k, j).wait_send()

        dr_copy(k).wait_send()

        @pl.when(k > 0)
        def _():
            dl_copy(k).wait_send()

        return carry

    lax.fori_loop(0, H, sent, 0)
    dr_copy(H).wait_send()
    for j in range(1, Y):
        y_copy(j).wait_send()
    for g in range(3):
        @pl.when(has_right)
        def _():
            to_right(g).wait_send()

        @pl.when(has_left)
        def _():
            to_left(g).wait_send()

    def left_out(k, carry):
        for j in range(1, Y):
            o_copy(k, j).wait_send()

        @pl.when(jnp.logical_not(is_own(k)))
        def _():
            o_copy(k, 0).wait_send()

        return carry

    lax.fori_loop(0, X, left_out, 0)


def layer(inputs, norm_gain, query_weight, key_weight, value_weight, query_gain, key_gain, out_weight):
    batch, L, D = inputs.shape
    Z, X, Y = (lax.axis_size(a) for a in ("z", "x", "y"))
    depth = query_weight.shape[0]
    parts = []
    for g in range(3):
        q, k, v = query_weight[:, g], key_weight[:, g], value_weight[:, g]
        parts += [q[:, 1], q[:, 0], v[:, 0], k[:, 0], k[:, 1], v[:, 1]]
    parts.append(out_weight.reshape(128, depth).T)
    weights = jnp.concatenate(parts, axis=1)
    scale = math.log2(math.e) / 8.0
    one = jnp.ones((64,), f32)
    tiles = []
    for g in range(3):
        tiles += [
            jnp.concatenate([query_gain[g], query_gain[g]]) * scale,
            jnp.concatenate([one, key_gain[g]]),
            jnp.concatenate([key_gain[g], one]),
        ]
    gains = jnp.stack(tiles)
    rows = X * L
    H = Z // 2
    dma = pltpu.SemaphoreType.DMA
    vmem = pl.BlockSpec(memory_space=pltpu.VMEM)
    cols = D // Y
    return pl.pallas_call(
        functools.partial(kernel, Z, X, Y, L),
        out_shape=jax.ShapeDtypeStruct((batch, L, cols), bf16),
        in_specs=[pl.BlockSpec(memory_space=pl.ANY), vmem, vmem, vmem],
        out_specs=vmem,
        scratch_shapes=[
            pltpu.VMEM((X, L, D), bf16),
            pltpu.VMEM((2, Z, X, 8, 1280), bf16),
            pltpu.VMEM((D, 1280), bf16),
            pltpu.VMEM((rows, D), bf16),
            pltpu.VMEM((3, rows, 128), bf16),
            *(pltpu.VMEM((2, rows + 2 * r, 128), bf16) for r in REACH),
            pltpu.VMEM((rows + 2 * REACH[2], 128), bf16),
            *(pltpu.VMEM((2, L, L + 2 * r), f32) for r in REACH),
            pltpu.VMEM((X, L, 128), bf16),
            pltpu.VMEM((Y, X, L, 128), bf16),
            pltpu.VMEM((Y, cols, 128), bf16),
            dma((X,)), dma((X,)), dma((X,)), dma((X,)), dma,
            dma((H, X)), dma((H, X)), dma((H, X)), dma((H, X)),
            dma((H + 1,)), dma((H + 1,)), dma((H + 1,)), dma((H + 1,)),
            dma((3, 2)), dma((3, 2)), dma((X, Y)), dma((Y, X)), dma((Y,)), dma((Y,)),
        ],
        compiler_params=pltpu.CompilerParams(
            collective_id=0, has_side_effects=True, vmem_limit_bytes=60 * 1024 * 1024
        ),
        name="layer",
    )(inputs, weights, norm_gain.reshape(1, D), gains)


def solution(mesh):
    count = mesh.shape["sp"]
    X = 4
    finer = Mesh(
        mesh.devices.reshape(count // (2 * X), X, 2, mesh.shape["tp"]), ("z", "x", "c", "y")
    )
    placed = (
        P(None, SP, None),
        P(),
        P(SP, None, "y", None),
        P(SP, None, "y", None),
        P(SP, None, "y", None),
        P(),
        P(),
        P("y", None, SP),
    )
    return jax.shard_map(
        layer, mesh=finer, in_specs=placed, out_specs=P(None, SP, "y"), check_vma=False
    )
```
